32 devices in a mesh: kv: 8 (over z, x), tp: 4 (over y, core).
Axes of the slice: x: 2, y: 2, z: 4, core: 2. Of those that a mesh axis runs over, the one named last changes fastest.
Arguments:
- inputs: bfloat16 [2048, 2048], P('kv', 'tp'), may hold values from -6 to 6
- queries: bfloat16 [2048, 2048], P('kv', 'tp'), may hold values from -8 to 8
- key_vectors: bfloat16 [2048, 512], P('kv', 'tp'), may hold values from -8 to 8
- value_rows_by_head: bfloat16 [2048, 512], P('kv', 'tp'), may hold values from -6 to 6
- out_grad: bfloat16 [2048, 2048], P('kv', 'tp'), may hold values from -6 to 6
- chosen: int32 [16, 16], replicated, may hold values from 0 to 31, as said below
Outputs:
- query_grad: bfloat16 [2048, 2048], P('kv', 'tp')
- key_grad: bfloat16 [2048, 512], P('kv', 'tp')
- value_grad: bfloat16 [2048, 512], P('kv', 'tp')
- weight_grad: float32 [2048, 2048], P('kv', 'tp')
The draws below stay inside these ranges and needn't reach their ends.
Inputs may be any that keep to these rules, and one draw needn't show every extreme that they name: `chosen`: row r holds 16 distinct key-block numbers, among them every key block that intersects query block r. The rows of one device (aligned runs of 2 rows) name at most 2 distinct key blocks that lie on any one other device (aligned runs of 4 key blocks), and exactly 2 at some other device for some devices.
All inputs are finite; a program needn't handle non-finite values.
Results may differ from the reference program's by a relative error of at most 0.015.
The reference program's roundings to bfloat16 on the way (of `probs_half` and `score_grad`) count: a program that leaves them out, or rounds other values in their place, can miss the bound.
Values may be sent and summed in bfloat16 or wider, within the bound.
No kernel may reach another device: no remote copies, remote signals or barrier semaphores. Data moves between devices by JAX's collectives and lax.ppermute only.
A program may use at most 128 MiB of HBM per device.

```python
import jax
import jax.numpy as jnp
from jax import lax

D = 2048
QUERY_HEADS = 32
KEY_VALUE_HEADS = 8
HEAD_SIZE = 64
QB = 128
KB = 64
NSEL = 16
TOK_DEV = 256
SEQUENCE_TOKENS = 2048


def draw_queries(key, part):
    final_result = jnp.clip(jax.random.normal(jax.random.fold_in(key, 1), (SEQUENCE_TOKENS, QUERY_HEADS * HEAD_SIZE), jnp.float32), -6.0, 6.0)
    return final_result.astype(jnp.bfloat16)


def draw_key_vectors(key, part):
    final_result = jnp.clip(jax.random.normal(jax.random.fold_in(key, 2), (SEQUENCE_TOKENS, KEY_VALUE_HEADS * HEAD_SIZE), jnp.float32), -6.0, 6.0)
    return final_result.astype(jnp.bfloat16)


def draw_chosen(key, part):
    q_count = SEQUENCE_TOKENS // QB
    k_count = SEQUENCE_TOKENS // KB
    ratio = QB // KB
    owner_blocks = TOK_DEV // KB
    local_blocks = TOK_DEV // QB
    n_dev = SEQUENCE_TOKENS // TOK_DEV
    q_index = jnp.arange(q_count, dtype=jnp.int32)[:, None]
    k_index = jnp.arange(k_count, dtype=jnp.int32)[None, :]
    dev_grid = jnp.arange(n_dev, dtype=jnp.int32)[:, None]
    own_grid = jnp.arange(n_dev, dtype=jnp.int32)[None, :]
    random_phase = jax.random.randint(jax.random.fold_in(key, 7), (n_dev, n_dev), 0, ratio)
    phase = jnp.where(own_grid == (dev_grid - 1) % n_dev, ratio - 1, jnp.where(own_grid == (dev_grid - n_dev // 2) % n_dev, 0, random_phase))
    query_dev = q_index // local_blocks
    key_owner = k_index // owner_blocks
    key_offset = k_index % owner_blocks
    permitted = (key_owner == query_dev) | (key_offset % ratio == phase[query_dev, key_owner])
    own_block = k_index // ratio == q_index
    forced = (k_index == q_index * ratio - 1) | (k_index == q_index * ratio - k_count // 2)
    causal = k_index < q_index * ratio
    tier = jnp.where(own_block, 3, jnp.where(forced, 2, jnp.where(causal, 1, 0)))
    tier = jnp.where(permitted, tier, -1)
    popular = jax.random.randint(jax.random.fold_in(key, 5), (k_count,), 0, 2) * 7
    row_keys = jax.random.split(jax.random.fold_in(key, 6), q_count)
    noise = jax.vmap(lambda one_key: jax.random.permutation(one_key, k_count))(row_keys)
    ranking = tier * (k_count * 8) + popular[None, :] * k_count + noise
    _, picked = lax.top_k(ranking, NSEL)
    return picked.astype(jnp.int32)


def levels(rng, dims, shards, least, largest):
    loudness = 1.0
    for dim, parts in shards:
        draws = jax.random.uniform(jax.random.fold_in(jax.random.fold_in(rng, 6), dim), (parts,), jnp.float32, least / len(shards), largest / len(shards))
        loudness = loudness * jnp.repeat(jnp.exp(draws), dims[dim] // parts).reshape((-1,) + (1,) * (len(dims) - 1 - dim))
    return loudness


def centred(stream_key, dims, deviation, limit, shards=(), kind=jnp.bfloat16):
    level = levels(stream_key, dims, shards, -0.22, 0.18) if shards else 1.0
    entries = jax.random.normal(stream_key, dims, jnp.float32) * deviation * level
    return jnp.minimum(jnp.maximum(entries, -limit), limit).astype(kind)


def setup_inputs(seed: int = 0) -> dict:
    streams_of = jax.random.split(jax.random.key(seed), 7)
    inputs = centred(streams_of[0], (SEQUENCE_TOKENS, D), 1.0, 6.0, ((0, 8), (1, 4)))
    queries = draw_queries(jax.random.fold_in(streams_of[6], 71), 0)
    key_vectors = draw_key_vectors(jax.random.fold_in(streams_of[6], 71), 0)
    value_rows_by_head = centred(streams_of[3], (SEQUENCE_TOKENS, KEY_VALUE_HEADS * HEAD_SIZE), 1.0, 6.0, ((0, 8), (1, 4)))
    out_grad = centred(streams_of[4], (SEQUENCE_TOKENS, QUERY_HEADS * HEAD_SIZE), 1.0, 6.0, ((0, 8), (1, 4)))
    chosen = draw_chosen(jax.random.fold_in(streams_of[6], 71), 0)
    return dict(inputs=inputs, queries=queries, key_vectors=key_vectors, value_rows_by_head=value_rows_by_head, out_grad=out_grad, chosen=chosen)


def round_trip(values_in):
    halved = lax.optimization_barrier(values_in.astype(jnp.bfloat16))
    return halved.astype(jnp.float32)


def reference(inputs, queries, key_vectors, value_rows_by_head, out_grad, chosen):
    total = queries.shape[0]
    q_heads = queries.shape[1] // HEAD_SIZE
    kv_heads = key_vectors.shape[1] // HEAD_SIZE
    group_size = q_heads // kv_heads
    score_scale = HEAD_SIZE ** -0.5
    offsets = jnp.arange(KB, dtype=jnp.int32)

    def step(state_pair, q_blk):
        acc_k, acc_v = state_pair
        first = q_blk * QB
        q_block = lax.dynamic_slice_in_dim(queries, first, QB, 0).astype(jnp.float32).reshape(QB, kv_heads, group_size, HEAD_SIZE)
        g_block = lax.dynamic_slice_in_dim(out_grad, first, QB, 0).astype(jnp.float32).reshape(QB, kv_heads, group_size, HEAD_SIZE)
        key_rows = (chosen[q_blk][:, None] * KB + offsets[None, :]).reshape(-1).astype(jnp.int32)
        key_sel = key_vectors[key_rows].astype(jnp.float32).reshape(-1, kv_heads, HEAD_SIZE)
        val_sel = value_rows_by_head[key_rows].astype(jnp.float32).reshape(-1, kv_heads, HEAD_SIZE)
        positions = first + jnp.arange(QB, dtype=jnp.int32)
        allowed = key_rows[None, :] <= positions[:, None]
        scores = jnp.einsum('tkgd,skd->kgts', q_block, key_sel) * score_scale
        scores = jnp.where(allowed, scores, -1e30)
        row_max = jnp.max(scores, axis=-1, keepdims=True)
        log_sum = row_max + jnp.log(jnp.sum(jnp.exp(scores - row_max), axis=-1, keepdims=True))
        probs = jnp.exp(scores - log_sum)
        probs_half = round_trip(probs)
        attended = jnp.einsum('kgts,skd->tkgd', probs_half, val_sel)
        row_dot = jnp.einsum('tkgd,tkgd->kgt', g_block, attended)
        prob_grad = jnp.einsum('tkgd,skd->kgts', g_block, val_sel)
        score_grad = round_trip(probs * (prob_grad - row_dot[..., None]))
        d_query = jnp.einsum('kgts,skd->tkgd', score_grad, key_sel) * score_scale
        d_key = jnp.einsum('kgts,tkgd->skd', score_grad, q_block) * score_scale
        d_value = jnp.einsum('kgts,tkgd->skd', probs_half, g_block)
        acc_k = acc_k.at[key_rows].add(d_key.reshape(-1, kv_heads * HEAD_SIZE))
        acc_v = acc_v.at[key_rows].add(d_value.reshape(-1, kv_heads * HEAD_SIZE))
        return (acc_k, acc_v), d_query.reshape(QB, q_heads * HEAD_SIZE)

    zeros = jnp.zeros((total, kv_heads * HEAD_SIZE), jnp.float32)
    (acc_k, acc_v), query_blocks = lax.scan(step, (zeros, zeros), jnp.arange(total // QB, dtype=jnp.int32))
    query_grad = query_blocks.reshape(total, q_heads * HEAD_SIZE).astype(jnp.bfloat16)
    weight_grad = jnp.dot(inputs.T, query_grad, preferred_element_type=jnp.float32)
    return query_grad, acc_k.astype(jnp.bfloat16), acc_v.astype(jnp.bfloat16), weight_grad
```

```python
import functools

import jax
import jax.numpy as jnp
from jax import lax
from jax.experimental import pallas as pl
from jax.experimental.pallas import tpu as pltpu
from jax.sharding import PartitionSpec as P

HEAD = 64
QB = 128
KB = 64


VMEM = pltpu.MemorySpace.VMEM
SMEM = pltpu.MemorySpace.SMEM
NT = (((1,), (1,)), ((), ()))
TN = (((0,), (0,)), ((), ()))
BF16, F32, I32 = jnp.bfloat16, jnp.float32, jnp.int32


def used_bits(chosen_ref, row, rows, owner, owner_blocks):
    bits = jnp.int32(0)
    for r in range(rows):
        for s in range(chosen_ref.shape[1]):
            e = chosen_ref[row + r, s]
            hit = e // owner_blocks == owner
            bits = bits | jnp.where(hit, jnp.int32(1) << (e % owner_blocks), 0)
    return bits


def nth_bit(bits, nth, owner_blocks):
    found, seen = jnp.int32(0), jnp.int32(0)
    for b in range(owner_blocks):
        bit = (bits >> b) & 1
        found = jnp.where((bit == 1) & (seen == nth), b, found)
        seen = seen + bit
    return found


def pack_kernel(n, local_blocks, heads, chosen_ref, k_ref, v_ref, *out):
    me = lax.axis_index("kv")
    owner_blocks = k_ref.shape[0] // KB
    sends, owns = out[:heads], out[heads:]
    for c in range(heads):
        lanes = slice(c * HEAD, (c + 1) * HEAD)
        owns[c][...] = jnp.concatenate([k_ref[:, lanes], v_ref[:, lanes]], axis=1)

    def to_one(j, _):
        bits = used_bits(chosen_ref, j * local_blocks, local_blocks, me, owner_blocks)
        for t in range(local_blocks):
            first = pl.multiple_of(nth_bit(bits, t, owner_blocks) * KB, KB)
            for c in range(heads):
                sends[c][j, t * KB : (t + 1) * KB, :] = owns[c][pl.ds(first, KB), :]
        return 0

    lax.fori_loop(0, n, to_one, 0)


def attend_kernel(
    n, local_blocks, group, chosen_ref, recv_ref, own_ref, q_ref, g_ref,
    dq_ref, back_ref, mine_ref,
    bits_ref, kv_s, s_s, dp_s, ph_s, ds_s, acc_s,
):
    me = lax.axis_index("kv")
    nsel = chosen_ref.shape[1]
    owner_blocks = own_ref.shape[0] // KB
    slots = local_blocks * KB
    tail = n * slots
    for o in range(n):
        bits_ref[o] = 0
    for r in range(local_blocks):
        for s in range(nsel):
            e = chosen_ref[me * local_blocks + r, s]
            o = e // owner_blocks
            bits_ref[o] = bits_ref[o] | (jnp.int32(1) << (e % owner_blocks))
    acc_s[...] = jnp.zeros_like(acc_s)
    lane = lax.broadcasted_iota(I32, (QB, 2 * HEAD), 1)
    ahead = lax.broadcasted_iota(I32, (KB, QB), 1) - lax.broadcasted_iota(I32, (KB, QB), 0)

    def one_block(r, _):
        row = me * local_blocks + r
        first = pl.multiple_of(r * QB, QB)
        offs, froms = [], []
        for s in range(nsel):
            e = chosen_ref[row, s]
            o, b = e // owner_blocks, e % owner_blocks
            bits = bits_ref[o]
            slot = jnp.int32(0)
            for i in range(owner_blocks - 1):
                slot = slot + jnp.where(i < b, (bits >> i) & 1, 0)
            local = o == me
            off = jnp.where(local, tail + b * KB, o * slots + slot * KB)
            offs.append(pl.multiple_of(off, KB))
            froms.append(e * KB - row * QB)

            @pl.when(local)
            def _():
                kv_s[s * KB : (s + 1) * KB, :] = own_ref[pl.ds(pl.multiple_of(b * KB, KB), KB), :]

            @pl.when(jnp.logical_not(local))
            def _():
                at = pl.multiple_of(o * slots + slot * KB, KB)
                kv_s[s * KB : (s + 1) * KB, :] = recv_ref[pl.ds(at, KB), :]

        q2, o2 = [], []
        for h in range(group):
            q = q_ref[pl.ds(first, QB), h * HEAD : (h + 1) * HEAD] * jnp.asarray(HEAD**-0.5, BF16)
            g = g_ref[pl.ds(first, QB), h * HEAD : (h + 1) * HEAD]
            z = jnp.zeros_like(q)
            q2.append(jnp.concatenate([q, z], axis=1))
            o2.append(jnp.concatenate([z, g], axis=1))
        q2 = jnp.concatenate(q2, axis=0)
        o2 = jnp.concatenate(o2, axis=0)
        keys = kv_s[...]
        s_s[...] = lax.dot_general(keys, q2, NT, preferred_element_type=F32)
        dp_s[...] = lax.dot_general(keys, o2, NT, preferred_element_type=F32)
        for h in range(group):
            cols = slice(h * QB, (h + 1) * QB)
            top = jnp.full((8, QB), -1e30, F32)
            for s in range(nsel):
                rows = slice(s * KB, (s + 1) * KB)
                x = jnp.where(ahead >= froms[s], s_s[rows, cols], -1e30)
                s_s[rows, cols] = x
                top = jnp.maximum(top, jnp.max(x.reshape(KB // 8, 8, QB), axis=0))
            top = jnp.max(top, axis=0, keepdims=True)
            total = jnp.zeros((8, QB), F32)
            for s in range(nsel):
                rows = slice(s * KB, (s + 1) * KB)
                x = jnp.exp(s_s[rows, cols] - top)
                s_s[rows, cols] = x
                total = total + jnp.sum(x.reshape(KB // 8, 8, QB), axis=0)
            scale = 1.0 / jnp.sum(total, axis=0, keepdims=True)
            dot = jnp.zeros((8, QB), F32)
            for s in range(nsel):
                rows = slice(s * KB, (s + 1) * KB)
                half = (s_s[rows, cols] * scale).astype(BF16)
                ph_s[rows, cols] = half
                y = half.astype(F32) * dp_s[rows, cols]
                dot = dot + jnp.sum(y.reshape(KB // 8, 8, QB), axis=0)
            dot = jnp.sum(dot, axis=0, keepdims=True)
            for s in range(nsel):
                rows = slice(s * KB, (s + 1) * KB)
                x = (s_s[rows, cols] * scale) * (dp_s[rows, cols] - dot)
                ds_s[rows, cols] = x.astype(BF16)
        dkv = jnp.dot(ds_s[...], q2, preferred_element_type=F32) + jnp.dot(
            ph_s[...], o2, preferred_element_type=F32
        )
        for s in range(nsel):
            acc_s[pl.ds(offs[s], KB), :] += dkv[s * KB : (s + 1) * KB]
        dqt = lax.dot_general(keys, ds_s[...], TN, preferred_element_type=F32)
        dq = jnp.transpose(dqt[:HEAD] * (HEAD**-0.5))
        for h in range(group):
            dq_ref[pl.ds(first, QB), h * HEAD : (h + 1) * HEAD] = dq[h * QB : (h + 1) * QB].astype(BF16)
        return 0

    lax.fori_loop(0, local_blocks, one_block, 0)
    back_ref[...] = acc_s[:tail, :].astype(BF16)
    mine_ref[...] = acc_s[tail:, :]


def join_kernel(n, local_blocks, heads, chosen_ref, *refs):
    me = lax.axis_index("kv")
    recvs, mines = refs[:heads], refs[heads : 2 * heads]
    dk_ref, dv_ref = refs[2 * heads : 2 * heads + 2]
    accs = refs[2 * heads + 2 :]
    owner_blocks = dk_ref.shape[0] // KB
    for c in range(heads):
        accs[c][...] = mines[c][...]

    def from_one(j, _):
        bits = used_bits(chosen_ref, j * local_blocks, local_blocks, me, owner_blocks)
        for t in range(local_blocks):
            first = pl.multiple_of(nth_bit(bits, t, owner_blocks) * KB, KB)
            for c in range(heads):
                accs[c][pl.ds(first, KB), :] += recvs[c][j, t * KB : (t + 1) * KB, :].astype(F32)
        return 0

    lax.fori_loop(0, n, from_one, 0)
    for c in range(heads):
        lanes = slice(c * HEAD, (c + 1) * HEAD)
        dk_ref[:, lanes] = accs[c][:, :HEAD].astype(BF16)
        dv_ref[:, lanes] = accs[c][:, HEAD:].astype(BF16)


def vspec():
    return pl.BlockSpec(memory_space=VMEM)


def sspec():
    return pl.BlockSpec(memory_space=SMEM)


def body(inputs, queries, key_vectors, value_rows_by_head, out_grad, chosen):
    n, tp = lax.axis_size("kv"), lax.axis_size("tp")
    rows_dev, cols = queries.shape
    heads = key_vectors.shape[1] // HEAD
    group = cols // HEAD // heads
    local_blocks = rows_dev // QB
    nsel = chosen.shape[1]
    slots = local_blocks * KB
    width = group * HEAD
    kv_i, tp_i = lax.axis_index("kv"), lax.axis_index("tp")

    packed = pl.pallas_call(
        functools.partial(pack_kernel, n, local_blocks, heads),
        out_shape=[jax.ShapeDtypeStruct((n, slots, 2 * HEAD), BF16)] * heads
        + [jax.ShapeDtypeStruct((rows_dev, 2 * HEAD), BF16)] * heads,
        in_specs=[sspec(), vspec(), vspec()],
        out_specs=[vspec()] * (2 * heads),
        name="pack",
    )(chosen, key_vectors, value_rows_by_head)
    sends, owns = packed[:heads], packed[heads:]
    recvs = [lax.all_to_all(x, "kv", 0, 0, tiled=True).reshape(n * slots, 2 * HEAD) for x in sends]

    half = n // 2
    flip = half | (half // 2)
    cs = tp // 2
    units = tp * n

    def spot(i, t):
        return i * tp + t

    first_perm, second_perm = [], []
    for i in range(n):
        for t in range(tp):
            top, y = i // half, t // cs
            if y == top:
                first_perm.append((spot(i, t), spot(i, t ^ cs)))
            else:
                first_perm.append((spot(i, t), spot(i ^ flip, t)))
                second_perm.append((spot(i, t), spot(i ^ flip, t ^ cs)))
    got1 = lax.ppermute(inputs, ("kv", "tp"), first_perm)
    got2 = lax.ppermute(inputs, ("kv", "tp"), second_perm)
    at_home = (tp_i // cs) == (kv_i // half)
    pair = jnp.concatenate([jnp.where(at_home, inputs, got1), jnp.where(at_home, got1, got2)], axis=0)
    pairs = [pair]
    for m in range(1, cs):
        pairs.append(lax.ppermute(pair, "tp", [(t, t ^ m) for t in range(tp)]))
    c_i = tp_i % cs
    spread = []
    for c in range(cs):
        x = pairs[0]
        for m in range(1, cs):
            x = jnp.where((c_i ^ m) == c, pairs[m], x)
        spread.append(x)

    dq, backs, mines = [], [], []
    for c in range(heads):
        flops = local_blocks * nsel * KB * group * QB * 2 * HEAD * 12
        out = pl.pallas_call(
            functools.partial(attend_kernel, n, local_blocks, group),
            grid=(1,),
            out_shape=[
                jax.ShapeDtypeStruct((rows_dev, width), BF16),
                jax.ShapeDtypeStruct((n * slots, 2 * HEAD), BF16),
                jax.ShapeDtypeStruct((rows_dev, 2 * HEAD), F32),
            ],
            in_specs=[
                sspec(), vspec(), vspec(),
                pl.BlockSpec((rows_dev, width), lambda i, c=c: (0, c)),
                pl.BlockSpec((rows_dev, width), lambda i, c=c: (0, c)),
            ],
            out_specs=[vspec()] * 3,
            scratch_shapes=[
                pltpu.SMEM((n,), I32),
                pltpu.VMEM((nsel * KB, 2 * HEAD), BF16),
                pltpu.VMEM((nsel * KB, group * QB), F32),
                pltpu.VMEM((nsel * KB, group * QB), F32),
                pltpu.VMEM((nsel * KB, group * QB), BF16),
                pltpu.VMEM((nsel * KB, group * QB), BF16),
                pltpu.VMEM((n * slots + rows_dev, 2 * HEAD), F32),
            ],
            cost_estimate=pl.CostEstimate(flops=flops, bytes_accessed=4 << 20, transcendentals=0),
            name="attend",
        )(chosen, recvs[c], owns[c], queries, out_grad)
        dq.append(out[0])
        backs.append(out[1])
        mines.append(out[2])

    landed = [lax.all_to_all(x.reshape(n, slots, 2 * HEAD), "kv", 0, 0, tiled=True) for x in backs]
    key_grad, value_grad = pl.pallas_call(
        functools.partial(join_kernel, n, local_blocks, heads),
        out_shape=[jax.ShapeDtypeStruct((rows_dev, heads * HEAD), BF16)] * 2,
        in_specs=[sspec()] + [vspec()] * (2 * heads),
        out_specs=[vspec()] * 2,
        scratch_shapes=[pltpu.VMEM((rows_dev, 2 * HEAD), F32)] * heads,
        name="join",
    )(chosen, *landed, *mines)

    groups = [list(range(half)), list(range(half, n))]
    pieces = []
    for c in range(heads):
        other = lax.ppermute(dq[c], "kv", [(i, i ^ flip) for i in range(n)])
        terms = []
        for x in spread:
            a = lax.dot_general(x[:rows_dev], dq[c], TN, preferred_element_type=F32)
            b = lax.dot_general(x[rows_dev:], other, TN, preferred_element_type=F32)
            terms.append((a + b).astype(BF16))
        term = jnp.concatenate(terms, axis=0).reshape(half, -1, width)
        got = lax.all_to_all(term, "kv", 0, 0, tiled=True, axis_index_groups=groups)
        pieces.append(jnp.sum(got.astype(F32), axis=0))
    weight_grad = jnp.concatenate(pieces, axis=1)
    return jnp.concatenate(dq, axis=1), key_grad, value_grad, weight_grad


def solution(mesh):
    placed = (P("kv", "tp"),) * 5 + (P(),)
    return jax.shard_map(
        body, mesh=mesh, in_specs=placed, out_specs=(P("kv", "tp"),) * 4, check_vma=False
    )
```

```python
import functools

import jax
import jax.numpy as jnp
from jax import lax
from jax.experimental import pallas as pl
from jax.experimental.pallas import tpu as pltpu
from jax.sharding import PartitionSpec as P


HEAD = 64
QB = 128
KB = 64


PACK_VMEM = 60 << 20
VMEM = pltpu.MemorySpace.VMEM
SMEM = pltpu.MemorySpace.SMEM
NT = (((1,), (1,)), ((), ()))
TN = (((0,), (0,)), ((), ()))
BF16, F32, I32 = jnp.bfloat16, jnp.float32, jnp.int32


def split(e, size):
    if size & (size - 1) == 0:
        return e >> (size.bit_length() - 1), e & (size - 1)
    return lax.div(e, jnp.int32(size)), lax.rem(e, jnp.int32(size))


def used_bits(chosen_ref, row, rows, owner, owner_blocks):
    bits = jnp.int32(0)
    for r in range(rows):
        for s in range(chosen_ref.shape[1]):
            e = chosen_ref[row + r, s]
            o, b = split(e, owner_blocks)
            bits = bits | jnp.where(o == owner, jnp.int32(1) << b, 0)
    return bits


def nth_bit(bits, nth, owner_blocks):
    found, seen = jnp.int32(0), jnp.int32(0)
    for b in range(owner_blocks):
        bit = (bits >> b) & 1
        found = jnp.where((bit == 1) & (seen == nth), b, found)
        seen = seen + bit
    return found


def own_kernel(heads, k_ref, v_ref, *owns):
    for c in range(heads):
        lanes = slice(c * HEAD, (c + 1) * HEAD)
        owns[c][...] = jnp.concatenate([k_ref[:, lanes], v_ref[:, lanes]], axis=1)


def pack_kernel(n, local_blocks, heads, chosen_ref, k_ref, v_ref, send_ref, table_ref, kv_s):
    me = lax.axis_index("kv")
    owner_blocks = k_ref.shape[0] // KB
    for c in range(heads):
        lanes = slice(c * HEAD, (c + 1) * HEAD)
        kv_s[:, 2 * c * HEAD : (2 * c + 1) * HEAD] = k_ref[:, lanes]
        kv_s[:, (2 * c + 1) * HEAD : (2 * c + 2) * HEAD] = v_ref[:, lanes]
    for d in range(1, n):
        j = me ^ d
        bits = used_bits(chosen_ref, j * local_blocks, local_blocks, me, owner_blocks)
        for t in range(local_blocks):
            nth = nth_bit(bits, t, owner_blocks)
            table_ref[d * local_blocks + t] = nth
            at = pl.multiple_of(nth * KB, KB)
            send_ref[j, t * KB : (t + 1) * KB, :] = kv_s[pl.ds(at, KB), :]


def attend_kernel(
    n, local_blocks, group, chosen_ref, own_ref, got_ref, q_ref, g_ref, *refs
):
    dq_ref, full_ref, back_ref, mine_ref = refs[-12:-8]
    bits_ref, recv_ref, kv_s, s_s, dp_s, ph_s, ds_s, acc_s = refs[-8:]
    me = lax.axis_index("kv")
    nsel = chosen_ref.shape[1]
    owner_blocks = own_ref.shape[0] // KB
    slots = local_blocks * KB
    tail = n * slots
    for o in range(n):
        bits_ref[o] = 0
    for r in range(local_blocks):
        for s in range(nsel):
            e = chosen_ref[me * local_blocks + r, s]
            o, b = split(e, owner_blocks)
            bits_ref[o] = bits_ref[o] | (jnp.int32(1) << b)
    acc_s[...] = jnp.zeros_like(acc_s)
    recv_ref[pl.ds(pl.multiple_of(tail, KB), own_ref.shape[0]), :] = own_ref[...]
    recv_ref[:tail, :] = got_ref[...]
    ahead = lax.broadcasted_iota(I32, (KB, QB), 1) - lax.broadcasted_iota(I32, (KB, QB), 0)

    def one_block(r, _):
        row = me * local_blocks + r
        first = pl.multiple_of(r * QB, QB)
        offs, froms = [], []
        for s in range(nsel):
            e = chosen_ref[row, s]
            o, b = split(e, owner_blocks)
            bits = bits_ref[o]
            slot = jnp.int32(0)
            for i in range(owner_blocks - 1):
                slot = slot + jnp.where(i < b, (bits >> i) & 1, 0)
            local = o == me
            off = jnp.where(local, tail + b * KB, o * slots + slot * KB)
            offs.append(pl.multiple_of(off, KB))
            froms.append(e * KB - row * QB)

            kv_s[s * KB : (s + 1) * KB, :] = recv_ref[pl.ds(offs[s], KB), :]

        q2, o2 = [], []
        for h in range(group):
            q = q_ref[pl.ds(first, QB), h * HEAD : (h + 1) * HEAD] * jnp.asarray(HEAD**-0.5, BF16)
            g = g_ref[pl.ds(first, QB), h * HEAD : (h + 1) * HEAD]
            z = jnp.zeros_like(q)
            q2.append(jnp.concatenate([q, z], axis=1))
            o2.append(jnp.concatenate([z, g], axis=1))
        q2 = jnp.concatenate(q2, axis=0)
        o2 = jnp.concatenate(o2, axis=0)
        keys = kv_s[...]
        s_s[...] = lax.dot_general(keys, q2, NT, preferred_element_type=F32)
        dp_s[...] = lax.dot_general(keys, o2, NT, preferred_element_type=F32)
        for h in range(group):
            cols = slice(h * QB, (h + 1) * QB)
            top = jnp.full((8, QB), -1e30, F32)
            for s in range(nsel):
                rows = slice(s * KB, (s + 1) * KB)
                x = jnp.where(ahead >= froms[s], s_s[rows, cols], -1e30)
                s_s[rows, cols] = x
                top = jnp.maximum(top, jnp.max(x.reshape(KB // 8, 8, QB), axis=0))
            top = jnp.max(top, axis=0, keepdims=True)
            total = jnp.zeros((8, QB), F32)
            for s in range(nsel):
                rows = slice(s * KB, (s + 1) * KB)
                x = jnp.exp(s_s[rows, cols] - top)
                s_s[rows, cols] = x
                total = total + jnp.sum(x.reshape(KB // 8, 8, QB), axis=0)
            scale = 1.0 / jnp.sum(total, axis=0, keepdims=True)
            dot = jnp.zeros((8, QB), F32)
            for s in range(nsel):
                rows = slice(s * KB, (s + 1) * KB)
                half = (s_s[rows, cols] * scale).astype(BF16)
                ph_s[rows, cols] = half
                y = half.astype(F32) * dp_s[rows, cols]
                dot = dot + jnp.sum(y.reshape(KB // 8, 8, QB), axis=0)
            dot = jnp.sum(dot, axis=0, keepdims=True)
            for s in range(nsel):
                rows = slice(s * KB, (s + 1) * KB)
                x = (s_s[rows, cols] * scale) * (dp_s[rows, cols] - dot)
                ds_s[rows, cols] = x.astype(BF16)
        dkv = jnp.dot(ds_s[...], q2, preferred_element_type=F32) + jnp.dot(
            ph_s[...], o2, preferred_element_type=F32
        )
        for s in range(nsel):
            acc_s[pl.ds(offs[s], KB), :] += dkv[s * KB : (s + 1) * KB]
        dqt = lax.dot_general(keys, ds_s[...], TN, preferred_element_type=F32)
        dq = jnp.transpose(dqt[:HEAD] * (HEAD**-0.5))
        for h in range(group):
            x = dq[h * QB : (h + 1) * QB].astype(BF16)
            dq_ref[pl.ds(first, QB), h * HEAD : (h + 1) * HEAD] = x
            full_ref[pl.ds(first, QB), h * HEAD : (h + 1) * HEAD] = x
        return 0

    lax.fori_loop(0, local_blocks, one_block, 0)
    back_ref[...] = acc_s[:tail, :].astype(BF16)
    mine_ref[...] = acc_s[tail:, :]


def join_kernel(n, local_blocks, heads, table_ref, *refs):
    me = lax.axis_index("kv")
    recvs, mines = refs[:heads], refs[heads : 2 * heads]
    dk_ref, dv_ref = refs[2 * heads : 2 * heads + 2]
    accs = refs[2 * heads + 2 :]
    for c in range(heads):
        accs[c][...] = mines[c][...]
    for d in range(1, n):
        for t in range(local_blocks):
            first = pl.multiple_of(table_ref[d * local_blocks + t] * KB, KB)
            for c in range(heads):
                accs[c][pl.ds(first, KB), :] += recvs[c][me ^ d, t * KB : (t + 1) * KB, :].astype(F32)
    for c in range(heads):
        lanes = slice(c * HEAD, (c + 1) * HEAD)
        dk_ref[:, lanes] = accs[c][:, :HEAD].astype(BF16)
        dv_ref[:, lanes] = accs[c][:, HEAD:].astype(BF16)


def term_kernel(half, cs, rows, dq_ref, other_ref, *refs):
    pairs = refs[:cs]
    own_ref, leaving, y_s = refs[cs], refs[cs + 1 : -1], refs[-1]
    c_i = lax.axis_index("tp") % cs
    place = lax.axis_index("kv") % half
    unit = pairs[0].shape[1]
    each = unit * cs // half
    for m in range(cs):
        y = lax.dot_general(pairs[m][:rows, :], dq_ref[...], TN, preferred_element_type=F32)
        y = y + lax.dot_general(pairs[m][rows:, :], other_ref[...], TN, preferred_element_type=F32)
        y_s[pl.ds(pl.multiple_of((c_i ^ m) * unit, unit), unit), :] = y
    for d in range(half):
        x = y_s[pl.ds(pl.multiple_of((place ^ d) * each, each), each), :]
        if d == 0:
            own_ref[...] = x
        else:
            leaving[d - 1][...] = x.astype(BF16)


def finish_kernel(half, heads, *refs):
    out_ref = refs[-1]
    width = out_ref.shape[1] // heads
    for c in range(heads):
        x = refs[c * half][...]
        for d in range(1, half):
            x = x + refs[c * half + d][...].astype(F32)
        out_ref[:, c * width : (c + 1) * width] = x


def vspec():
    return pl.BlockSpec(memory_space=VMEM)


def sspec():
    return pl.BlockSpec(memory_space=SMEM)


def body(inputs, queries, key_vectors, value_rows_by_head, out_grad, chosen):
    n, tp = lax.axis_size("kv"), lax.axis_size("tp")
    rows_dev, cols = queries.shape
    heads = key_vectors.shape[1] // HEAD
    group = cols // HEAD // heads
    local_blocks = rows_dev // QB
    nsel = chosen.shape[1]
    slots = local_blocks * KB
    width = group * HEAD
    kv_i, tp_i = lax.axis_index("kv"), lax.axis_index("tp")

    wide = 2 * HEAD
    send, table = pl.pallas_call(
        functools.partial(pack_kernel, n, local_blocks, heads),
        out_shape=[
            jax.ShapeDtypeStruct((n, slots, wide * heads), BF16),
            jax.ShapeDtypeStruct((n * local_blocks,), I32),
        ],
        in_specs=[sspec(), vspec(), vspec()],
        out_specs=[vspec(), sspec()],
        scratch_shapes=[pltpu.VMEM((rows_dev, wide * heads), BF16)],
        compiler_params=pltpu.CompilerParams(vmem_limit_bytes=PACK_VMEM),
        name="pack",
    )(chosen, key_vectors, value_rows_by_head)
    owns = pl.pallas_call(
        functools.partial(own_kernel, heads),
        out_shape=[jax.ShapeDtypeStruct((rows_dev, wide), BF16)] * heads,
        in_specs=[vspec(), vspec()],
        out_specs=[vspec()] * heads,
        compiler_params=pltpu.CompilerParams(vmem_limit_bytes=4 << 20),
        cost_estimate=pl.CostEstimate(flops=1 << 30, bytes_accessed=1 << 20, transcendentals=0),
        name="own",
    )(key_vectors, value_rows_by_head)
    recv = lax.all_to_all(send, "kv", 0, 0, tiled=True).reshape(n * slots, wide * heads)
    recv, inputs = lax.optimization_barrier((recv, inputs))

    half = n // 2
    flip = half | (half // 2)
    cs = tp // 2

    def spot(i, t):
        return i * tp + t

    first_perm = []
    for i in range(n):
        for t in range(tp):
            top, y = i // half, t // cs
            if y == top:
                first_perm.append((spot(i, t), spot(i, t ^ cs)))
            else:
                first_perm.append((spot(i, t), spot(i ^ flip, t)))
    got1 = lax.ppermute(inputs, ("kv", "tp"), first_perm)
    got2 = lax.ppermute(got1, "tp", [(t, t ^ cs) for t in range(tp)])
    at_home = (tp_i // cs) == (kv_i // half)
    pair = jnp.concatenate([jnp.where(at_home, inputs, got1), jnp.where(at_home, got1, got2)], axis=0)
    pairs = [pair]
    for m in range(1, cs):
        pairs.append(lax.ppermute(pair, "tp", [(t, t ^ m) for t in range(tp)]))

    dq, mines, kept, landed = [], [], [], []
    for c in range(heads):
        flops = local_blocks * nsel * KB * group * QB * wide * 12
        here = pl.BlockSpec((rows_dev, width), lambda i, c=c: (0, c))
        out = pl.pallas_call(
            functools.partial(attend_kernel, n, local_blocks, group),
            grid=(1,),
            out_shape=[
                jax.ShapeDtypeStruct((rows_dev, width), BF16),
                jax.ShapeDtypeStruct((rows_dev, cols), BF16),
                jax.ShapeDtypeStruct((n * slots, wide), BF16),
                jax.ShapeDtypeStruct((rows_dev, wide), F32),
            ],
            in_specs=[
                sspec(), vspec(), pl.BlockSpec((n * slots, wide), lambda i, c=c: (0, c)), here, here
            ]
            + [pl.BlockSpec(memory_space=pl.ANY)] * len(kept),
            out_specs=[vspec(), here, vspec(), vspec()],
            input_output_aliases={5: 1} if kept else {},
            scratch_shapes=[
                pltpu.SMEM((n,), I32),
                pltpu.VMEM((n * slots + rows_dev, wide), BF16),
                pltpu.VMEM((nsel * KB, wide), BF16),
                pltpu.VMEM((nsel * KB, group * QB), F32),
                pltpu.VMEM((nsel * KB, group * QB), F32),
                pltpu.VMEM((nsel * KB, group * QB), BF16),
                pltpu.VMEM((nsel * KB, group * QB), BF16),
                pltpu.VMEM((n * slots + rows_dev, wide), F32),
            ],
            compiler_params=pltpu.CompilerParams(vmem_limit_bytes=24 << 20),
            cost_estimate=pl.CostEstimate(flops=flops, bytes_accessed=4 << 20, transcendentals=0),
        )(chosen, owns[c], recv, queries, out_grad, *kept)
        dq.append(out[0])
        kept = [out[1]]
        mines.append(out[3])
        landed.append(lax.all_to_all(out[2].reshape(n, slots, wide), "kv", 0, 0, tiled=True))
    query_grad = kept[0]

    key_grad, value_grad = pl.pallas_call(
        functools.partial(join_kernel, n, local_blocks, heads),
        out_shape=[jax.ShapeDtypeStruct((rows_dev, heads * HEAD), BF16)] * 2,
        in_specs=[sspec()] + [vspec()] * (2 * heads),
        out_specs=[vspec()] * 2,
        scratch_shapes=[pltpu.VMEM((rows_dev, wide), F32)] * heads,
        compiler_params=pltpu.CompilerParams(vmem_limit_bytes=8 << 20),
        name="join",
    )(table, *landed, *mines)

    each = inputs.shape[1] * tp // n
    gathered = []
    for c in range(heads):
        other = lax.ppermute(dq[c], "kv", [(i, i ^ flip) for i in range(n)])
        terms = pl.pallas_call(
            functools.partial(term_kernel, half, cs, rows_dev),
            out_shape=[jax.ShapeDtypeStruct((each, width), F32)]
            + [jax.ShapeDtypeStruct((each, width), BF16)] * (half - 1),
            in_specs=[vspec()] * (2 + cs),
            out_specs=[vspec()] * half,
            scratch_shapes=[pltpu.VMEM((each * half, width), F32)],
            compiler_params=pltpu.CompilerParams(vmem_limit_bytes=12 << 20),
            cost_estimate=pl.CostEstimate(
                flops=4 * rows_dev * each * half * width, bytes_accessed=2 << 20, transcendentals=0
            ),
        )(dq[c], other, *pairs)
        gathered.append(terms[0])
        for d in range(1, half):
            gathered.append(lax.ppermute(terms[d], "kv", [(i, i ^ d) for i in range(n)]))
    weight_grad = pl.pallas_call(
        functools.partial(finish_kernel, half, heads),
        out_shape=jax.ShapeDtypeStruct((each, cols), F32),
        in_specs=[vspec()] * (half * heads),
        out_specs=vspec(),
        compiler_params=pltpu.CompilerParams(vmem_limit_bytes=8 << 20),
        name="finish",
    )(*gathered)
    return query_grad, key_grad, value_grad, weight_grad


def solution(mesh):

    placed = (P("kv", "tp"),) * 5 + (P(),)
    return jax.shard_map(
        body, mesh=mesh, in_specs=placed, out_specs=(P("kv", "tp"),) * 4, check_vma=False
    )
```

```python
import functools

import jax
import jax.numpy as jnp
from jax import lax
from jax.experimental import pallas as pl
from jax.experimental.pallas import tpu as pltpu
from jax.sharding import PartitionSpec as P


HEAD = 64
QB = 128
KB = 64


VMEM = pltpu.MemorySpace.VMEM
SMEM = pltpu.MemorySpace.SMEM
NT = (((1,), (1,)), ((), ()))
TN = (((0,), (0,)), ((), ()))
BF16, F32, I32 = jnp.bfloat16, jnp.float32, jnp.int32


def split(e, size):
    if size & (size - 1) == 0:
        return e >> (size.bit_length() - 1), e & (size - 1)
    return lax.div(e, jnp.int32(size)), lax.rem(e, jnp.int32(size))


def used_bits(chosen_ref, row, rows, owner, owner_blocks):
    bits = jnp.int32(0)
    for r in range(rows):
        for s in range(chosen_ref.shape[1]):
            e = chosen_ref[row + r, s]
            o, b = split(e, owner_blocks)
            bits = bits | jnp.where(o == owner, jnp.int32(1) << b, 0)
    return bits


def nth_bit(bits, nth, owner_blocks):
    found, seen = jnp.int32(0), jnp.int32(0)
    for b in range(owner_blocks):
        bit = (bits >> b) & 1
        found = jnp.where((bit == 1) & (seen == nth), b, found)
        seen = seen + bit
    return found


def picks_kernel(n, near, local_blocks, owner_blocks, chosen_ref, picks_ref):
    me = lax.axis_index("kv")
    for f in range(1, n // near):
        j = me ^ (f * near)
        for m in range(near):
            bits = used_bits(chosen_ref, j * local_blocks, local_blocks, me ^ m, owner_blocks)
            for t in range(local_blocks):
                picks_ref[(f * near + m) * local_blocks + t] = nth_bit(bits, t, owner_blocks)


def pack_kernel(n, near, local_blocks, heads, picks_ref, *refs):
    me = lax.axis_index("kv")
    keys, values, sends = refs[:near], refs[near : 2 * near], refs[2 * near :]
    slots = local_blocks * KB
    for f in range(1, n // near):
        for m in range(near):
            place = (me ^ m) % near
            for t in range(local_blocks):
                at = pl.multiple_of(picks_ref[(f * near + m) * local_blocks + t] * KB, KB)
                to = pl.multiple_of(place * slots + t * KB, KB)
                k, v = keys[m][pl.ds(at, KB), :], values[m][pl.ds(at, KB), :]
                for c in range(heads):
                    lanes = slice(c * HEAD, (c + 1) * HEAD)
                    x = jnp.concatenate([k[:, lanes], v[:, lanes]], axis=1)
                    sends[f - 1][pl.ds(to, KB), 2 * c * HEAD : 2 * (c + 1) * HEAD] = x


def attend_kernel(n, near, local_blocks, group, head, chosen_ref, q_ref, g_ref, *refs):
    keys, values, far_refs = refs[:near], refs[near : 2 * near], refs[2 * near : 2 * near + n // near - 1]
    outs = refs[-(n // near + 10) : -8]
    dq_ref, full_ref, close_ref, back_refs = outs[0], outs[1], outs[2], outs[3:]
    bits_ref, recv_ref, kv_s, s_s, dp_s, ph_s, ds_s, acc_s = refs[-8:]
    me = lax.axis_index("kv")
    nsel = chosen_ref.shape[1]
    rows_dev = keys[0].shape[0]
    lanes = slice(head * HEAD, (head + 1) * HEAD)
    owner_blocks = rows_dev // KB
    slots = local_blocks * KB
    tail = n * slots
    for o in range(n):
        bits_ref[o] = 0
    for r in range(local_blocks):
        for s in range(nsel):
            e = chosen_ref[me * local_blocks + r, s]
            o, b = split(e, owner_blocks)
            bits_ref[o] = bits_ref[o] | (jnp.int32(1) << b)
    acc_s[...] = jnp.zeros_like(acc_s)
    for m in range(near):
        at = pl.multiple_of(tail + ((me ^ m) % near) * rows_dev, KB)
        recv_ref[pl.ds(at, rows_dev), :] = jnp.concatenate([keys[m][:, lanes], values[m][:, lanes]], axis=1)
    for f in range(1, n // near):
        at = pl.multiple_of((me // near ^ f) * (near * slots), KB)
        recv_ref[pl.ds(at, near * slots), :] = far_refs[f - 1][...]
    ahead = lax.broadcasted_iota(I32, (KB, QB), 1) - lax.broadcasted_iota(I32, (KB, QB), 0)

    def one_block(r, _):
        row = me * local_blocks + r
        first = pl.multiple_of(r * QB, QB)
        offs, froms = [], []
        for s in range(nsel):
            e = chosen_ref[row, s]
            o, b = split(e, owner_blocks)
            bits = bits_ref[o]
            slot = jnp.int32(0)
            for i in range(owner_blocks - 1):
                slot = slot + jnp.where(i < b, (bits >> i) & 1, 0)
            close = o // near == me // near
            off = jnp.where(close, tail + (o % near) * rows_dev + b * KB, o * slots + slot * KB)
            offs.append(pl.multiple_of(off, KB))
            froms.append(e * KB - row * QB)

            kv_s[s * KB : (s + 1) * KB, :] = recv_ref[pl.ds(offs[s], KB), :]

        q2, o2 = [], []
        for h in range(group):
            q = q_ref[pl.ds(first, QB), h * HEAD : (h + 1) * HEAD] * jnp.asarray(HEAD**-0.5, BF16)
            g = g_ref[pl.ds(first, QB), h * HEAD : (h + 1) * HEAD]
            z = jnp.zeros_like(q)
            q2.append(jnp.concatenate([q, z], axis=1))
            o2.append(jnp.concatenate([z, g], axis=1))
        q2 = jnp.concatenate(q2, axis=0)
        o2 = jnp.concatenate(o2, axis=0)
        keys = kv_s[...]
        s_s[...] = lax.dot_general(keys, q2, NT, preferred_element_type=F32)
        dp_s[...] = lax.dot_general(keys, o2, NT, preferred_element_type=F32)
        for h in range(group):
            cols = slice(h * QB, (h + 1) * QB)
            top = jnp.full((8, QB), -1e30, F32)
            for s in range(nsel):
                rows = slice(s * KB, (s + 1) * KB)
                x = jnp.where(ahead >= froms[s], s_s[rows, cols], -1e30)
                s_s[rows, cols] = x
                top = jnp.maximum(top, jnp.max(x.reshape(KB // 8, 8, QB), axis=0))
            top = jnp.max(top, axis=0, keepdims=True)
            total = jnp.zeros((8, QB), F32)
            for s in range(nsel):
                rows = slice(s * KB, (s + 1) * KB)
                x = jnp.exp(s_s[rows, cols] - top)
                s_s[rows, cols] = x
                total = total + jnp.sum(x.reshape(KB // 8, 8, QB), axis=0)
            scale = 1.0 / jnp.sum(total, axis=0, keepdims=True)
            dot = jnp.zeros((8, QB), F32)
            for s in range(nsel):
                rows = slice(s * KB, (s + 1) * KB)
                half = (s_s[rows, cols] * scale).astype(BF16)
                ph_s[rows, cols] = half
                y = half.astype(F32) * dp_s[rows, cols]
                dot = dot + jnp.sum(y.reshape(KB // 8, 8, QB), axis=0)
            dot = jnp.sum(dot, axis=0, keepdims=True)
            for s in range(nsel):
                rows = slice(s * KB, (s + 1) * KB)
                x = (s_s[rows, cols] * scale) * (dp_s[rows, cols] - dot)
                ds_s[rows, cols] = x.astype(BF16)
        dkv = jnp.dot(ds_s[...], q2, preferred_element_type=F32) + jnp.dot(
            ph_s[...], o2, preferred_element_type=F32
        )
        for s in range(nsel):
            acc_s[pl.ds(offs[s], KB), :] += dkv[s * KB : (s + 1) * KB]
        dqt = lax.dot_general(keys, ds_s[...], TN, preferred_element_type=F32)
        dq = jnp.transpose(dqt[:HEAD] * (HEAD**-0.5))
        for h in range(group):
            x = dq[h * QB : (h + 1) * QB].astype(BF16)
            dq_ref[pl.ds(first, QB), h * HEAD : (h + 1) * HEAD] = x
            full_ref[pl.ds(first, QB), h * HEAD : (h + 1) * HEAD] = x
        return 0

    lax.fori_loop(0, local_blocks, one_block, 0)
    close_ref[...] = acc_s[tail:, :]
    for f in range(1, n // near):
        at = pl.multiple_of((me // near ^ f) * (near * slots), KB)
        back_refs[f - 1][...] = acc_s[pl.ds(at, near * slots), :].astype(BF16)


def relay_kernel(n, near, local_blocks, heads, picks_ref, *refs):
    me = lax.axis_index("kv")
    fars, closes = refs[: n // near - 1], refs[n // near - 1 : n // near - 1 + heads]
    outs, acc = refs[-near - 1 : -1], refs[-1]
    wide, slots, rows_dev = 2 * HEAD, local_blocks * KB, closes[0].shape[0] // near
    for c in range(heads):
        acc[:, c * wide : (c + 1) * wide] = closes[c][...]
    for f in range(1, n // near):
        for m in range(near):
            place = (me ^ m) % near
            for t in range(local_blocks):
                at = place * rows_dev + picks_ref[(f * near + m) * local_blocks + t] * KB
                to = pl.ds(pl.multiple_of(at, KB), KB)
                rows = pl.ds(pl.multiple_of(place * slots + t * KB, KB), KB)
                acc[to, :] += fars[f - 1][rows, :].astype(F32)
    for m in range(near):
        x = acc[pl.ds(pl.multiple_of((me ^ m) % near * rows_dev, KB), rows_dev), :]
        outs[m][...] = x if m == 0 else x.astype(BF16)


def join_kernel(near, heads, *refs):
    dk_ref, dv_ref = refs[near:]
    x = refs[0][...]
    for m in range(1, near):
        x = x + refs[m][...].astype(F32)
    for c in range(heads):
        lanes = slice(c * HEAD, (c + 1) * HEAD)
        dk_ref[:, lanes] = x[:, 2 * c * HEAD : (2 * c + 1) * HEAD].astype(BF16)
        dv_ref[:, lanes] = x[:, (2 * c + 1) * HEAD : (2 * c + 2) * HEAD].astype(BF16)


def term_kernel(half, near, near_first, cs, dq_ref, other_ref, *refs):
    pairs, outs, y_s = refs[: 2 * cs], refs[2 * cs : -1], refs[-1]
    c_i = lax.axis_index("tp") % cs
    place = lax.axis_index("kv") % half
    unit = pairs[0].shape[1]
    each = unit * cs // half
    for m in range(cs):
        y = lax.dot_general(pairs[2 * m][...], dq_ref[...], TN, preferred_element_type=F32)
        y = y + lax.dot_general(pairs[2 * m + 1][...], other_ref[...], TN, preferred_element_type=F32)
        y_s[pl.ds(pl.multiple_of((c_i ^ m) * unit, unit), unit), :] = y
    far = half // near
    first, second = (near, far) if near_first else (far, near)
    for i in range(first):
        for j in range(second):
            d = i + near * j if near_first else near * i + j
            x = y_s[pl.ds(pl.multiple_of((place ^ d) * each, each), each), :]
            outs[i][j * each : (j + 1) * each, :] = x if i == 0 else x.astype(BF16)


def add_kernel(first, second, *refs):
    each = refs[0].shape[0] // second
    for j in range(second):
        rows = slice(j * each, (j + 1) * each)
        x = refs[0][rows, :]
        for i in range(1, first):
            x = x + refs[i][rows, :].astype(F32)
        refs[first + j][...] = x if j == 0 else x.astype(BF16)


def finish_kernel(counts, *refs):
    out_ref = refs[-1]
    width = out_ref.shape[1] // len(counts)
    k = 0
    for c, count in enumerate(counts):
        x = refs[k][...]
        for i in range(1, count):
            x = x + refs[k + i][...].astype(F32)
        out_ref[:, c * width : (c + 1) * width] = x
        k += count


def vspec():
    return pl.BlockSpec(memory_space=VMEM)


def sspec():
    return pl.BlockSpec(memory_space=SMEM)


def body(inputs, queries, key_vectors, value_rows_by_head, out_grad, chosen):
    n, tp = lax.axis_size("kv"), lax.axis_size("tp")
    rows_dev, cols = queries.shape
    heads = key_vectors.shape[1] // HEAD
    group = cols // HEAD // heads
    local_blocks = rows_dev // QB
    nsel = chosen.shape[1]
    slots = local_blocks * KB
    width = group * HEAD
    kv_i, tp_i = lax.axis_index("kv"), lax.axis_index("tp")

    wide = 2 * HEAD
    near = 1 << ((n.bit_length() - 1) // 2)
    owner_blocks = rows_dev // KB
    keys, values = [key_vectors], [value_rows_by_head]
    for m in range(1, near):
        keys.append(lax.ppermute(key_vectors, "kv", [(i, i ^ m) for i in range(n)]))
        values.append(lax.ppermute(value_rows_by_head, "kv", [(i, i ^ m) for i in range(n)]))
    picks = pl.pallas_call(
        functools.partial(picks_kernel, n, near, local_blocks, owner_blocks),
        out_shape=jax.ShapeDtypeStruct((n * local_blocks,), I32),
        in_specs=[sspec()],
        out_specs=sspec(),
        compiler_params=pltpu.CompilerParams(vmem_limit_bytes=4 << 20),
        cost_estimate=pl.CostEstimate(flops=1 << 28, bytes_accessed=1 << 10, transcendentals=0),
        name="picks",
    )(chosen)
    sends = pl.pallas_call(
        functools.partial(pack_kernel, n, near, local_blocks, heads),
        out_shape=[jax.ShapeDtypeStruct((near * slots, wide * heads), BF16)] * (n // near - 1),
        in_specs=[sspec()] + [vspec()] * (2 * near),
        out_specs=[vspec()] * (n // near - 1),
        compiler_params=pltpu.CompilerParams(vmem_limit_bytes=8 << 20),
        name="pack",
    )(picks, *keys, *values)
    fars = []
    for f in range(1, n // near):
        fars.append(lax.ppermute(sends[f - 1], "kv", [(i, i ^ (f * near)) for i in range(n)]))

    half = n // 2
    flip = half | (half // 2)
    cs = tp // 2

    beside = lax.ppermute(inputs, "tp", [(t, t ^ cs) for t in range(tp)])
    at_home = (tp_i // cs) == (kv_i // half)
    mine = jnp.where(at_home, inputs, beside)
    theirs = jnp.where(at_home, beside, inputs)
    theirs, mine, fars = lax.optimization_barrier((theirs, mine, fars))
    theirs = lax.ppermute(theirs, "kv", [(i, i ^ flip) for i in range(n)])
    dq, closes, kept = [], [], []
    back_shape = jax.ShapeDtypeStruct((near * slots, wide * heads), BF16)
    for c in range(heads):
        flops = local_blocks * nsel * KB * group * QB * wide * 12
        here = pl.BlockSpec((rows_dev, width), lambda i, c=c: (0, c))
        out = pl.pallas_call(
            functools.partial(attend_kernel, n, near, local_blocks, group, c),
            grid=(1,),
            out_shape=[
                jax.ShapeDtypeStruct((rows_dev, width), BF16),
                jax.ShapeDtypeStruct((rows_dev, cols), BF16),
                jax.ShapeDtypeStruct((near * rows_dev, wide), F32),
            ]
            + [back_shape] * (n // near - 1),
            in_specs=[
                sspec(), here, here
            ]
            + [vspec()] * (2 * near)
            + [pl.BlockSpec((near * slots, wide), lambda i, c=c: (0, c))] * (n // near - 1)
            + [pl.BlockSpec(memory_space=pl.ANY)] * len(kept),
            out_specs=[vspec(), here, vspec()]
            + [pl.BlockSpec((near * slots, wide), lambda i, c=c: (0, c))] * (n // near - 1),
            input_output_aliases={2 + 2 * near + n // near + i: 1 + i + (i > 0) for i in range(len(kept))},
            scratch_shapes=[
                pltpu.SMEM((n,), I32),
                pltpu.VMEM((n * slots + near * rows_dev, wide), BF16),
                pltpu.VMEM((nsel * KB, wide), BF16),
                pltpu.VMEM((nsel * KB, group * QB), F32),
                pltpu.VMEM((nsel * KB, group * QB), F32),
                pltpu.VMEM((nsel * KB, group * QB), BF16),
                pltpu.VMEM((nsel * KB, group * QB), BF16),
                pltpu.VMEM((n * slots + near * rows_dev, wide), F32),
            ],
            compiler_params=pltpu.CompilerParams(vmem_limit_bytes=24 << 20),
            cost_estimate=pl.CostEstimate(flops=flops, bytes_accessed=4 << 20, transcendentals=0),
        )(chosen, queries, out_grad, *keys, *values, *fars, *kept)
        dq.append(out[0])
        kept = [out[1], *out[3:]]
        closes.append(out[2])
    mine, dq[0] = lax.optimization_barrier((mine, dq[0]))
    pairs = [mine, theirs]
    for m in range(1, cs):
        pairs.append(lax.ppermute(mine, "tp", [(t, t ^ m) for t in range(tp)]))
        pairs.append(lax.ppermute(theirs, "tp", [(t, t ^ m) for t in range(tp)]))

    query_grad, backs = kept[0], kept[1:]

    landed = []
    for f in range(1, n // near):
        landed.append(lax.ppermute(backs[f - 1], "kv", [(i, i ^ (f * near)) for i in range(n) if i > i ^ (f * near)]))
    relayed = list(
        pl.pallas_call(
            functools.partial(relay_kernel, n, near, local_blocks, heads),
            out_shape=[jax.ShapeDtypeStruct((rows_dev, wide * heads), F32)]
            + [jax.ShapeDtypeStruct((rows_dev, wide * heads), BF16)] * (near - 1),
            in_specs=[sspec()] + [vspec()] * (n // near - 1 + heads),
            out_specs=[vspec()] * near,
            scratch_shapes=[pltpu.VMEM((near * rows_dev, wide * heads), F32)],
            compiler_params=pltpu.CompilerParams(vmem_limit_bytes=12 << 20),
            name="relay",
        )(picks, *landed, *closes)
    )
    for m in range(1, near):
        relayed[m] = lax.ppermute(relayed[m], "kv", [(i, i ^ m) for i in range(n)])
    key_grad, value_grad = pl.pallas_call(
        functools.partial(join_kernel, near, heads),
        out_shape=[jax.ShapeDtypeStruct((rows_dev, heads * HEAD), BF16)] * 2,
        in_specs=[vspec()] * near,
        out_specs=[vspec()] * 2,
        compiler_params=pltpu.CompilerParams(vmem_limit_bytes=8 << 20),
        name="join",
    )(*relayed)

    each = inputs.shape[1] * tp // n
    gathered, counts = [], []
    for c in range(heads):
        near_first = True
        inner = half // near
        first, second = (near, inner) if near_first else (inner, near)
        step1, step2 = (1, near) if near_first else (near, 1)
        other = lax.ppermute(dq[c], "kv", [(i, i ^ flip) for i in range(n)])
        terms = pl.pallas_call(
            functools.partial(term_kernel, half, near, near_first, cs),
            out_shape=[jax.ShapeDtypeStruct((second * each, width), F32)]
            + [jax.ShapeDtypeStruct((second * each, width), BF16)] * (first - 1),
            in_specs=[vspec()] * (2 + 2 * cs),
            out_specs=[vspec()] * first,
            scratch_shapes=[pltpu.VMEM((each * half, width), F32)],
            compiler_params=pltpu.CompilerParams(vmem_limit_bytes=12 << 20),
            cost_estimate=pl.CostEstimate(
                flops=4 * rows_dev * each * half * width, bytes_accessed=2 << 20, transcendentals=0
            ),
        )(dq[c], other, *pairs)
        terms = list(terms)
        for i in range(1, first):
            d = i * step1
            terms[i] = lax.ppermute(terms[i], "kv", [(j, j ^ d) for j in range(n)])
        sums = pl.pallas_call(
            functools.partial(add_kernel, first, second),
            out_shape=[jax.ShapeDtypeStruct((each, width), F32)]
            + [jax.ShapeDtypeStruct((each, width), BF16)] * (second - 1),
            in_specs=[vspec()] * first,
            out_specs=[vspec()] * second,
            compiler_params=pltpu.CompilerParams(vmem_limit_bytes=8 << 20),
        )(*terms)
        sums = list(sums)
        for i in range(1, second):
            d = i * step2
            sums[i] = lax.ppermute(sums[i], "kv", [(j, j ^ d) for j in range(n)])
        gathered += sums
        counts.append(second)
    weight_grad = pl.pallas_call(
        functools.partial(finish_kernel, counts),
        out_shape=jax.ShapeDtypeStruct((each, cols), F32),
        in_specs=[vspec()] * len(gathered),
        out_specs=vspec(),
        compiler_params=pltpu.CompilerParams(vmem_limit_bytes=8 << 20),
        name="finish",
    )(*gathered)
    return query_grad, key_grad, value_grad, weight_grad


def solution(mesh):

    placed = (P("kv", "tp"),) * 5 + (P(),)
    return jax.shard_map(
        body, mesh=mesh, in_specs=placed, out_specs=(P("kv", "tp"),) * 4, check_vma=False
    )
```
